32 devices in a mesh: sp: 8 (over z, x), tp: 4 (over y, core).
Axes of the slice: x: 2, y: 2, z: 4, core: 2. Of those that a mesh axis runs over, the one named last changes fastest.
Arguments:
- skip_stream_entering: bfloat16 [1024, 2048], P('sp', 'tp'), may hold values from -24 to 24
- unfiltered_channel_feed: bfloat16 [1024, 2048], P('sp', 'tp'), may hold values from -6 to 6
- unfiltered_state_entry: bfloat16 [1024, 2048], P('sp', 'tp'), may hold values from -6 to 6
- unfiltered_state_exit: bfloat16 [1024, 2048], P('sp', 'tp'), may hold values from -6 to 6
- final_valve_preactivation: bfloat16 [1024, 2048], P('sp', 'tp'), may hold values from -6 to 6
- increment_preactivation: float32 [2, 32, 1024], P(None, 'tp', 'sp'), may hold values from -8 to 8
- summed_attenuation_both_ways: float32 [2, 32, 1024], P(None, 'tp', 'sp'), may hold values from -0.7 to 0, as said below
- channel_fading_speed: float32 [2, 32], P(None, 'tp'), may hold values from 0.0001953125 to 0.03, as said below
- channel_feed_filter: float32 [5, 2048], P(None, 'tp'), may hold values from -2.5 to 2.5
- state_entry_filter: float32 [5, 2048], P(None, 'tp'), may hold values from -2.5 to 2.5
- state_exit_filter: float32 [5, 2048], P(None, 'tp'), may hold values from -2.5 to 2.5
- clustered_rescale_factor: float32 [2048], P('tp'), may hold values from 0.1 to 1.9
- final_projection_weights: bfloat16 [2048, 2048], P(None, 'tp'), may hold values from -0.125 to 0.125
- specialist_rescale_factor: float32 [2048], replicated, may hold values from 0.1 to 1.9
- item_specialist_couple: int32 [1024, 2], P('sp'), may hold values from 0 to 7, all different within a row; in each aligned block of 128 rows (0 to 127, 128 to 255, ...) at most 64 rows name the same one
- selected_cluster_likelihood: float32 [1024], P('sp'), may hold values from 0.3 to 1
- selected_twin_scores_raw: float32 [1024, 2], P('sp'), may hold values from -6 to 6
- specialist_gating_weights: bfloat16 [8, 2048, 4096], P('sp', None, 'tp'), may hold values from -0.125 to 0.125
- specialist_raising_weights: bfloat16 [8, 2048, 4096], P('sp', None, 'tp'), may hold values from -0.125 to 0.125
- specialist_lowering_weights: bfloat16 [8, 4096, 2048], P('sp', 'tp'), may hold values from -0.09375 to 0.09375
Outputs:
- layer_out: bfloat16 [1024, 2048], P('sp', 'tp')
The draws below stay inside these ranges and needn't reach their ends.
Inputs may be any that keep to these rules, and one draw needn't show every extreme that they name: For every head, dt times channel_fading_speed at the rate of the draw sets how far a state is carried; summed_attenuation_both_ways holds a few sharp losses of state. `summed_attenuation_both_ways`: mostly zero. `item_specialist_couple`: the two experts of a row differ. Among the rows of one index of sp (aligned blocks of 128 rows) no expert is named by more than 64 rows, a bound that some expert reaches in some blocks.
All inputs are finite; a program needn't handle non-finite values.
Results may differ from the reference program's by a relative error of at most 0.0095.
Values may be sent and summed in bfloat16 or wider, within the bound.
A program may use at most 64 MiB of HBM per device.

```python
import math
import jax
import jax.numpy as jnp
import numpy as np
from jax import lax

D = 2048
HEADS = 32
HD = 64
GROUPS = 16
NS = 128
CONV = 5
D_EXPERT = 4096
TOP = 2
TOK_DEV = 128
TOKENS = 1024
INNER = 2048
EXPERTS = 8
CAP = 64
N_TP = 4


def draw_channel_fading_speed(key, part):
    uniform_part = jax.random.uniform(key, (2, HEADS), jnp.float32)
    lowest = 0.2 / TOKENS
    highest = 0.03
    return jnp.exp(math.log(lowest) + uniform_part * (math.log(highest) - math.log(lowest)))


def draw_increment_preactivation(key, part):
    first_key, second_key = jax.random.split(key)
    base = jax.random.normal(first_key, (2, HEADS, TOKENS), jnp.float32)
    offsets = jax.random.uniform(second_key, (2, 1, TOKENS // TOK_DEV), jnp.float32, -1.0, 1.0)
    offsets = jnp.repeat(offsets, TOK_DEV, axis=2)
    values = base + offsets
    return jnp.clip(values, -8.0, 8.0)


def draw_summed_attenuation_both_ways(key, part):
    first_key, second_key = jax.random.split(key)
    chosen = jax.random.randint(first_key, (2, HEADS, TOKENS), 0, TOKENS) < 3
    amount = jax.random.uniform(second_key, (2, HEADS, TOKENS), jnp.float32, 0.22, 0.69)
    return jnp.where(chosen, -amount, 0.0)


def draw_skip_stream_entering(key, part):
    first_key, second_key = jax.random.split(key, 2)
    base = jax.random.normal(first_key, (TOKENS, D), jnp.float32)
    columns = jnp.exp(math.log(4.0) * jnp.arange(D, dtype=jnp.float32) / D)
    row_scale = jax.random.uniform(second_key, (TOKENS, 1), jnp.float32, 0.6, 1.6)
    values = base * row_scale * columns
    return jnp.clip(values, -24.0, 24.0).astype(jnp.bfloat16)


def block_levels(key, extent, cuts, low, top_value):
    gain, own = 1.0, jax.random.fold_in(key, 6)
    for axis_at, blocks in cuts:
        heights = jnp.exp(jax.random.uniform(jax.random.fold_in(own, axis_at), (blocks,), jnp.float32, low / len(cuts), top_value / len(cuts)))
        gain = gain * jnp.repeat(heights, extent[axis_at] // blocks).reshape([-1 if axis == axis_at else 1 for axis in range(len(extent))])
    return gain


def deal_out(key, own, number, rows, count, top, bound, lean):
    order = jax.random.permutation(key, count)
    packed, ordinary = portions_of(count, rows * top, bound, lean, True), portions_of(count, rows * top, bound, lean, False)
    places = jnp.arange(count)

    def named(tallies, rotation):
        used = int((tallies > 0).sum())
        fixed = max(1, used // 4)
        shifted = fixed + (places - fixed + rotation * (used - fixed)) % max(1, count - fixed)
        return jnp.zeros((count,), jnp.int32).at[order[jnp.where(places < fixed, places, shifted)]].set(jnp.asarray(tallies, jnp.int32))

    tallies = jnp.where(number % 4 == 0, named(packed, number // 4), named(ordinary, number - number // 4 - 1))
    mixed = jax.random.permutation(jax.random.fold_in(own, 3), count)
    source_of, receiver = mixed[0:count // 2 * 2:2], mixed[1:count // 2 * 2:2]
    room = jnp.minimum(tallies[source_of] - 1, bound - tallies[receiver]) // 2
    room = jnp.where((source_of == order[0]) | (receiver == order[0]) | (tallies[receiver] == 0), 0, jnp.maximum(room, 0))
    shifted = jax.random.randint(jax.random.fold_in(own, 4), (count // 2,), 0, 1 << 20) % (room + 1)
    tallies = tallies.at[source_of].add(-shifted).at[receiver].add(shifted)
    labels = jnp.searchsorted(jnp.cumsum(tallies), jnp.arange(rows * top), side="right").astype(jnp.int32)
    table = labels.reshape(top, rows).T
    table = table[jax.random.permutation(jax.random.fold_in(own, 1), rows)]
    rotation = jax.random.randint(jax.random.fold_in(own, 2), (rows, 1), 0, top)
    return jnp.take_along_axis(table, (jnp.arange(top)[None, :] + rotation) % top, axis=1)


def portions_of(number_of, total, reach, skew, full):
    loads = [(1 << 20) // math.isqrt(grade ** skew) + 1 for grade in range(1, number_of + 1)]
    largest = reach if full else min(reach, max(-(-total // number_of), total * loads[0] // sum(loads)))
    least = 1 if total - largest >= number_of - 1 else 0
    counts, surplus = [largest] + [least] * (number_of - 1), total - largest - least * (number_of - 1)
    while surplus > 0:
        free = [i for i in range(1, number_of) if counts[i] < largest] or [i for i in range(1, number_of) if counts[i] < reach]
        whole, budget = sum([loads[i] for i in free]), surplus
        for i in free:
            more = min(reach - counts[i], max(1, budget * loads[i] // whole), surplus)
            counts[i] = counts[i] + more
            surplus = surplus - more
    return np.array(counts)


def noise(rng, shape, deviation, most, cuts=(), held_as=jnp.bfloat16):
    values = deviation * jax.random.normal(rng, shape, jnp.float32)
    if cuts:
        values = values * block_levels(rng, shape, cuts, -0.22, 0.18)
    return jnp.clip(values, -most, most).astype(held_as)


def setup_inputs(seed: int = 0) -> dict:
    key_of = jax.random.split(jax.random.key(seed), 21)
    skip_stream_entering = draw_skip_stream_entering(jax.random.fold_in(key_of[20], 71), 0)
    unfiltered_channel_feed = noise(key_of[1], (TOKENS, INNER), 1.0, 6.0, ((0, 8), (1, 4)))
    unfiltered_state_entry = noise(key_of[2], (TOKENS, GROUPS * NS), 1.0, 6.0, ((0, 8), (1, 4)))
    unfiltered_state_exit = noise(key_of[3], (TOKENS, GROUPS * NS), 1.0, 6.0, ((0, 8), (1, 4)))
    final_valve_preactivation = noise(key_of[4], (TOKENS, INNER), 1.0, 6.0, ((0, 8), (1, 4)))
    increment_preactivation = draw_increment_preactivation(jax.random.fold_in(key_of[20], 71), 0)
    summed_attenuation_both_ways = draw_summed_attenuation_both_ways(jax.random.fold_in(key_of[20], 71), 0)
    channel_fading_speed = draw_channel_fading_speed(jax.random.fold_in(key_of[20], 71), 0)
    channel_feed_filter = noise(key_of[8], (CONV, INNER), CONV ** -0.5, 2.5, ((1, 4),), jnp.float32)
    state_entry_filter = noise(key_of[9], (CONV, GROUPS * NS), CONV ** -0.5, 2.5, ((1, 4),), jnp.float32)
    state_exit_filter = noise(key_of[10], (CONV, GROUPS * NS), CONV ** -0.5, 2.5, ((1, 4),), jnp.float32)
    clustered_rescale_factor = jnp.clip(1.0 + 0.18 * jax.random.normal(key_of[11], (INNER,), jnp.float32), 0.1, 1.9)
    final_projection_weights = noise(key_of[12], (INNER, D), INNER ** -0.5, 0.125, ((1, 4),))
    specialist_rescale_factor = jnp.clip(1.0 + 0.18 * jax.random.normal(key_of[13], (D,), jnp.float32), 0.1, 1.9)
    item_specialist_couple_keys = jax.random.split(jax.random.fold_in(key_of[14], 1), TOKENS // TOK_DEV)
    item_specialist_couple_turns = jax.random.permutation(jax.random.fold_in(key_of[14], 3), TOKENS // TOK_DEV)
    item_specialist_couple = jax.vmap(lambda own, number: deal_out(jax.random.fold_in(key_of[14], 2), own, number, TOK_DEV, EXPERTS, TOP, CAP, 1))(item_specialist_couple_keys, item_specialist_couple_turns).reshape((TOKENS, TOP))
    selected_cluster_likelihood = jnp.clip(0.3 + 0.7 * jax.random.uniform(key_of[15], (TOKENS,), jnp.float32) ** block_levels(key_of[15], (TOKENS,), ((0, 8),), -0.2, 0.2), 0.3, 1.0)
    selected_twin_scores_raw = noise(key_of[16], (TOKENS, TOP), 1.5, 6.0, ((0, 8),), jnp.float32)
    specialist_gating_weights = noise(key_of[17], (EXPERTS, D, D_EXPERT), D ** -0.5, 0.125, ((0, 8), (2, 4)))
    specialist_raising_weights = noise(key_of[18], (EXPERTS, D, D_EXPERT), D ** -0.5, 0.125, ((0, 8), (2, 4)))
    specialist_lowering_weights = noise(key_of[19], (EXPERTS, D_EXPERT, D), D_EXPERT ** -0.5, 0.09375, ((0, 8), (1, 4)))
    return {"skip_stream_entering": skip_stream_entering, "unfiltered_channel_feed": unfiltered_channel_feed, "unfiltered_state_entry": unfiltered_state_entry, "unfiltered_state_exit": unfiltered_state_exit, "final_valve_preactivation": final_valve_preactivation, "increment_preactivation": increment_preactivation, "summed_attenuation_both_ways": summed_attenuation_both_ways, "channel_fading_speed": channel_fading_speed, "channel_feed_filter": channel_feed_filter, "state_entry_filter": state_entry_filter, "state_exit_filter": state_exit_filter, "clustered_rescale_factor": clustered_rescale_factor, "final_projection_weights": final_projection_weights, "specialist_rescale_factor": specialist_rescale_factor, "item_specialist_couple": item_specialist_couple, "selected_cluster_likelihood": selected_cluster_likelihood, "selected_twin_scores_raw": selected_twin_scores_raw, "specialist_gating_weights": specialist_gating_weights, "specialist_raising_weights": specialist_raising_weights, "specialist_lowering_weights": specialist_lowering_weights}


HIGHEST = lax.Precision.HIGHEST
group_eps = 1e-05
stream_eps = 1e-06

def conv_silu(values, kernel):
    tap_count = kernel.shape[0]
    half_taps = tap_count // 2
    length = values.shape[0]
    padded = jnp.pad(values.astype(jnp.float32), ((half_taps, half_taps), (0, 0)))
    summed = jnp.zeros(values.shape, jnp.float32)
    for offset in range(tap_count):
        summed = summed + kernel[offset].astype(jnp.float32) * padded[offset:offset + length]
    return jax.nn.silu(summed).astype(jnp.bfloat16)

def block_parts(x_block, b_block, c_block, step_f, step_b, log_f, log_b):
    head_count = x_block.shape[1]
    group_count = b_block.shape[1]
    per_group = head_count // group_count
    length = x_block.shape[0]
    group_scores = jnp.einsum('tgn,sgn->gts', c_block, b_block, precision=HIGHEST)
    scores = jnp.repeat(group_scores, per_group, axis=0)
    b_head = jnp.repeat(b_block, per_group, axis=1)
    c_head = jnp.repeat(c_block, per_group, axis=1)
    forward = jnp.cumsum(log_f, axis=1)
    backward = jnp.flip(jnp.cumsum(jnp.flip(log_b, 1), axis=1), 1)
    row_index = lax.broadcasted_iota(jnp.int32, (length, length), 0)
    col_index = lax.broadcasted_iota(jnp.int32, (length, length), 1)
    lower_mask = (col_index <= row_index)[None]
    upper_mask = (col_index >= row_index)[None]
    decay_fwd = jnp.where(lower_mask, jnp.exp(jnp.minimum(forward[:, :, None] - forward[:, None, :], 0.0)), 0.0)
    decay_bwd = jnp.where(upper_mask, jnp.exp(jnp.minimum(backward[:, :, None] - backward[:, None, :], 0.0)), 0.0)
    mixing = scores * (decay_fwd * step_f[:, None, :] + decay_bwd * step_b[:, None, :])
    within = jnp.einsum('hts,shp->thp', mixing, x_block, precision=HIGHEST)
    weight_fwd = jnp.exp(forward[:, -1:] - forward) * step_f
    weight_bwd = jnp.exp(backward[:, :1] - backward) * step_b
    state_fwd = jnp.einsum('hs,shp,shn->hpn', weight_fwd, x_block, b_head, precision=HIGHEST)
    state_bwd = jnp.einsum('hs,shp,shn->hpn', weight_bwd, x_block, b_head, precision=HIGHEST)
    return (within, state_fwd, state_bwd, forward[:, -1], backward[:, 0], jnp.exp(forward), jnp.exp(backward), c_head)

def read_state(c_head, factor, state):
    return jnp.einsum('thn,hpn->thp', c_head, state, precision=HIGHEST) * jnp.transpose(factor)[:, :, None]

def carry_step(carried, items):
    state, total = items
    return (carried * jnp.exp(total)[:, None, None] + state, carried)

def reference(skip_stream_entering, unfiltered_channel_feed, unfiltered_state_entry, unfiltered_state_exit, final_valve_preactivation, increment_preactivation, summed_attenuation_both_ways, channel_fading_speed, channel_feed_filter, state_entry_filter, state_exit_filter, clustered_rescale_factor, final_projection_weights, specialist_rescale_factor, item_specialist_couple, selected_cluster_likelihood, selected_twin_scores_raw, specialist_gating_weights, specialist_raising_weights, specialist_lowering_weights):
    length = skip_stream_entering.shape[0]
    blocks = length // TOK_DEV
    x_conv = conv_silu(unfiltered_channel_feed, channel_feed_filter).astype(jnp.float32).reshape(blocks, TOK_DEV, HEADS, HD)
    b_conv = conv_silu(unfiltered_state_entry, state_entry_filter).astype(jnp.float32).reshape(blocks, TOK_DEV, GROUPS, NS)
    c_conv = conv_silu(unfiltered_state_exit, state_exit_filter).astype(jnp.float32).reshape(blocks, TOK_DEV, GROUPS, NS)
    whole_increment_list = jax.nn.softplus(increment_preactivation)
    whole_attenuation_list = -whole_increment_list * channel_fading_speed[:, :, None] + summed_attenuation_both_ways

    def split_blocks(array):
        return jnp.moveaxis(array.reshape(HEADS, blocks, TOK_DEV), 1, 0)

    def one_block(items):
        return block_parts(*items)
    parts = lax.map(one_block, (x_conv, b_conv, c_conv, split_blocks(whole_increment_list[0]), split_blocks(whole_increment_list[1]), split_blocks(whole_attenuation_list[0]), split_blocks(whole_attenuation_list[1])))
    within, state_fwd, state_bwd, total_fwd, total_bwd, factor_fwd, factor_bwd, c_head = parts
    zero_state = jnp.zeros((HEADS, HD, NS), jnp.float32)
    _, incoming_fwd = lax.scan(carry_step, zero_state, (state_fwd, total_fwd))
    _, incoming_bwd = lax.scan(carry_step, zero_state, (state_bwd, total_bwd), reverse=True)
    readout = jax.vmap(read_state)(c_head, factor_fwd, incoming_fwd) + jax.vmap(read_state)(c_head, factor_bwd, incoming_bwd)
    mixer_out = (within + readout).reshape(length, HEADS * HD)
    gated = mixer_out * jax.nn.silu(final_valve_preactivation.astype(jnp.float32))
    grouped = gated.reshape(length, GROUPS, -1)
    grouped = grouped * lax.rsqrt(lax.optimization_barrier(jnp.mean(grouped * grouped, axis=-1, keepdims=True)) + group_eps)
    mixed = (grouped.reshape(length, HEADS * HD) * clustered_rescale_factor).astype(jnp.bfloat16)
    stream = (skip_stream_entering.astype(jnp.float32) + jnp.dot(mixed, final_projection_weights, preferred_element_type=jnp.float32)).astype(jnp.bfloat16)
    stream_f = stream.astype(jnp.float32)
    normal = (stream_f * lax.rsqrt(lax.optimization_barrier(jnp.mean(stream_f * stream_f, axis=-1, keepdims=True)) + stream_eps) * specialist_rescale_factor).astype(jnp.bfloat16)
    first = jax.nn.sigmoid(selected_twin_scores_raw[:, 0] - selected_twin_scores_raw[:, 1])
    route_weight = selected_cluster_likelihood[:, None] * jnp.stack([first, 1.0 - first], axis=1)
    slot_total = blocks * CAP
    piece_width = D_EXPERT // N_TP

    def expert_step(summed, expert):
        matched = item_specialist_couple == expert
        row_hit = jnp.any(matched, axis=1)
        order = jnp.argsort(1 - row_hit.astype(jnp.int32), stable=True)[:slot_total]
        valid = row_hit[order].astype(jnp.float32)
        token_weight = lax.optimization_barrier(jnp.sum(jnp.where(matched, route_weight, 0.0), axis=1))
        rows = normal[order]
        gate = jnp.dot(rows, specialist_gating_weights[expert], preferred_element_type=jnp.float32)
        upward = jnp.dot(rows, specialist_raising_weights[expert], preferred_element_type=jnp.float32)
        hidden = (jax.nn.silu(gate) * upward).astype(jnp.bfloat16)
        down = specialist_lowering_weights[expert]

        def add_piece(total, index):
            start = index * piece_width
            hidden_piece = lax.dynamic_slice_in_dim(hidden, start, piece_width, 1)
            down_piece = lax.dynamic_slice_in_dim(down, start, piece_width, 0)
            partial_value = jnp.dot(hidden_piece, down_piece, preferred_element_type=jnp.float32).astype(jnp.bfloat16)
            return (total + partial_value.astype(jnp.float32), None)
        answer_f, _ = lax.scan(add_piece, jnp.zeros((slot_total, D), jnp.float32), jnp.arange(N_TP, dtype=jnp.int32))
        answer = answer_f.astype(jnp.bfloat16)
        scaled = answer.astype(jnp.float32) * (token_weight[order] * valid)[:, None]
        return (summed.at[order].add(scaled), None)
    experts_sum, _ = lax.scan(expert_step, jnp.zeros((length, D), jnp.float32), jnp.arange(EXPERTS, dtype=jnp.int32))
    return (stream_f + experts_sum).astype(jnp.bfloat16)
```

```python
import functools

import jax
import jax.numpy as jnp
from jax import lax
from jax.experimental import pallas as pl
from jax.experimental.pallas import tpu as pltpu
from jax.sharding import PartitionSpec as P

D = 2048
HD = 64
NS = 128
CONV = 5


HIGHEST = lax.Precision.HIGHEST
group_eps = 1e-05
stream_eps = 1e-06


def extended(cells, sides, width):
    for axis, dim in sides:
        count = lax.axis_size(axis)
        ends = count - 1
        head = lax.slice_in_dim(cells, 0, width, axis=dim)
        tail = lax.slice_in_dim(cells, cells.shape[dim] - width, cells.shape[dim], axis=dim)
        cells = jnp.concatenate(
            [
                lax.ppermute(tail, axis, [(i, (i + 1) % count) for i in range(ends)]),
                cells,
                lax.ppermute(head, axis, [((i + 1) % count, i) for i in range(ends)]),
            ],
            axis=dim,
        )
    return cells


def entering(shard, axis, join, neutral, backward):
    count = lax.axis_size(axis)
    place = lax.axis_index(axis)
    ahead = count - 1 - place if backward else place
    gathered = jax.tree.map(
        lambda a, kind: lax.all_gather(a.astype(kind), axis), shard, (jnp.bfloat16, jnp.bfloat16)
    )
    state = jax.tree.map(lambda a, e: jnp.zeros_like(a) + jnp.asarray(e, a.dtype), shard, neutral)

    def one(turn, state):
        source = count - 1 - turn if backward else turn
        return join(
            state,
            jax.tree.map(
                lambda a, own: lax.dynamic_index_in_dim(a, source, 0, False).astype(own.dtype),
                gathered,
                shard,
            ),
        )

    return lax.fori_loop(0, ahead, one, state)


def block_parts(x_short, b_short, c_short, step_f, step_b, log_f, log_b):
    head_count = x_short.shape[1]
    group_count = b_short.shape[1]
    per_group = head_count // group_count
    length = x_short.shape[0]
    group_scores = jnp.einsum("tgn,sgn->gts", c_short, b_short, preferred_element_type=jnp.float32)
    x_block = x_short.astype(jnp.float32)
    b_block = b_short.astype(jnp.float32)
    c_block = c_short.astype(jnp.float32)
    scores = jnp.repeat(group_scores, per_group, axis=0)
    b_head = jnp.repeat(b_block, per_group, axis=1)
    c_head = jnp.repeat(c_block, per_group, axis=1)
    forward = jnp.cumsum(log_f, axis=1)
    backward = jnp.flip(jnp.cumsum(jnp.flip(log_b, 1), axis=1), 1)
    row_index = lax.broadcasted_iota(jnp.int32, (length, length), 0)
    col_index = lax.broadcasted_iota(jnp.int32, (length, length), 1)
    lower_mask = (col_index <= row_index)[None]
    upper_mask = (col_index >= row_index)[None]
    decay_fwd = jnp.where(
        lower_mask, jnp.exp(jnp.minimum(forward[:, :, None] - forward[:, None, :], 0.0)), 0.0
    )
    decay_bwd = jnp.where(
        upper_mask, jnp.exp(jnp.minimum(backward[:, :, None] - backward[:, None, :], 0.0)), 0.0
    )
    mixing = scores * (decay_fwd * step_f[:, None, :] + decay_bwd * step_b[:, None, :])
    within = jnp.einsum("hts,shp->thp", mixing, x_block, precision=HIGHEST)
    weight_fwd = jnp.exp(forward[:, -1:] - forward) * step_f
    weight_bwd = jnp.exp(backward[:, :1] - backward) * step_b
    state_fwd = jnp.einsum("hs,shp,shn->hpn", weight_fwd, x_block, b_head, precision=HIGHEST)
    state_bwd = jnp.einsum("hs,shp,shn->hpn", weight_bwd, x_block, b_head, precision=HIGHEST)
    return (
        within,
        state_fwd,
        state_bwd,
        forward[:, -1],
        backward[:, 0],
        jnp.exp(forward),
        jnp.exp(backward),
        c_head,
    )


def read_state(c_head, factor, state):
    return (
        jnp.einsum("thn,hpn->thp", c_head, state, precision=HIGHEST)
        * jnp.transpose(factor)[:, :, None]
    )


def compose(earlier, later):
    return (earlier[0] + later[0], earlier[1] * jnp.exp(later[0])[:, None, None] + later[1])


MESH = pl.DeviceIdType.MESH
F32 = jnp.float32
BF16 = jnp.bfloat16


def remote(src, dst, send, recv, device):
    return pltpu.make_async_remote_copy(
        src_ref=src, dst_ref=dst, send_sem=send, recv_sem=recv, device_id=device, device_id_type=MESH
    )


def expert_kernel(
    count,
    tps,
    cap,
    stream_ref,
    selector_ref,
    high_ref,
    low_ref,
    gain_ref,
    gate_hbm,
    up_hbm,
    down_hbm,
    out_ref,
    gate_ref,
    up_ref,
    down_ref,
    leaving,
    rows,
    hidden,
    part,
    pair_in,
    pair_out,
    ring_in,
    answer,
    returned,
    weight_sem,
    a_send,
    a_recv,
    b_send,
    b_recv,
    p_send,
    p_recv,
    q_send,
    q_recv,
    r_send,
    r_recv,
):
    me = lax.axis_index("sp")
    mine = lax.axis_index("tp")
    halves = tps // 2
    tall = mine // 2
    core = mine % 2
    mate = tall * 2 + (1 - core)
    cols = stream_ref.shape[1]
    loads = [
        pltpu.make_async_copy(gate_hbm.at[0], gate_ref, weight_sem.at[0]),
        pltpu.make_async_copy(up_hbm.at[0], up_ref, weight_sem.at[1]),
        pltpu.make_async_copy(down_hbm.at[0], down_ref, weight_sem.at[2]),
    ]
    for load in loads:
        load.start()

    barrier = pltpu.get_barrier_semaphore()
    for k in range(1, count):
        pl.semaphore_signal(
            barrier, inc=1, device_id={"sp": (me + k) % count, "tp": mine}, device_id_type=MESH
        )
    for j in range(1, tps):
        pl.semaphore_signal(
            barrier, inc=1, device_id={"sp": me, "tp": (mine + j) % tps}, device_id_type=MESH
        )
    stream = stream_ref[...]
    sent = jnp.dot(selector_ref[...], stream, preferred_element_type=F32).astype(BF16)
    leaving[...] = sent
    rows[mine, 0:cap, :] = sent[0:cap]
    pl.semaphore_wait(barrier, count + tps - 2)

    pending = []

    def go(copy):
        copy.start()
        pending.append(copy)

    for k in range(1, count):
        go(
            remote(
                leaving.at[pl.ds(k * cap, cap), :],
                rows.at[mine, pl.ds(k * cap, cap), :],
                a_send.at[k],
                a_recv.at[k],
                {"sp": (me + k) % count, "tp": mine},
            )
        )

    batches = min(count, 8)
    span = count // batches

    def area(owner, batch):
        return rows.at[owner, pl.ds(batch * span * cap, span * cap), :]

    def arrived_from(owner, batch, index):
        remote(
            area(owner, batch),
            area(owner, batch),
            b_send.at[index, batch],
            b_recv.at[index, batch],
            {"tp": mate},
        ).wait_recv()

    def relay(batch):
        for j in range(1, halves):
            owner = ((tall + halves - j) % halves) * 2 + core
            arrived_from(owner, batch, j)
            go(
                remote(
                    area(owner, batch),
                    area(owner, batch),
                    b_send.at[halves + j, batch],
                    b_recv.at[halves + j, batch],
                    {"tp": mate},
                )
            )

    for batch in range(batches):
        for k in range(batch * span, (batch + 1) * span):
            if k > 0:
                spot = rows.at[mine, pl.ds(k * cap, cap), :]
                remote(spot, spot, a_send.at[k], a_recv.at[k], {"tp": mate}).wait_recv()
        for j in range(1, halves):
            go(
                remote(
                    area(mine, batch),
                    area(mine, batch),
                    b_send.at[j, batch],
                    b_recv.at[j, batch],
                    {"tp": ((tall + j) % halves) * 2 + core},
                )
            )
        go(
            remote(
                area(mine, batch),
                area(mine, batch),
                b_send.at[halves, batch],
                b_recv.at[halves, batch],
                {"tp": mate},
            )
        )
        if batch > 0:
            relay(batch - 1)
    relay(batches - 1)
    for batch in range(batches):
        for j in range(halves):
            arrived_from(((tall + halves - j) % halves) * 2 + 1 - core, batch, halves + j)
    for copy in pending:
        copy.wait_send()
    pending = []

    chunks = 2
    size = count * cap // chunks
    units = gate_ref.shape[1]
    tile = min(256, units)
    for load in loads:
        load.wait()

    def compute(chunk):
        lo = chunk * size
        squares = jnp.zeros((size, 1), F32)
        for t in range(tps):
            piece = rows[t, lo : lo + size, :].astype(F32)
            squares = squares + jnp.sum(piece * piece, axis=1, keepdims=True)
        scale = lax.rsqrt(squares / (tps * cols) + stream_eps)
        for t in range(tps):
            piece = rows[t, lo : lo + size, :].astype(F32)
            gain = gain_ref[:, t * cols : (t + 1) * cols]
            rows[t, lo : lo + size, :] = (piece * scale * gain).astype(BF16)

        @pl.loop(0, units // tile)
        def _(step):
            where = pl.ds(pl.multiple_of(step * tile, tile), tile)
            gate = jnp.zeros((size, tile), F32)
            upward = jnp.zeros((size, tile), F32)
            for t in range(tps):
                piece = rows[t, lo : lo + size, :]
                ins = slice(t * cols, (t + 1) * cols)
                gate = gate + jnp.dot(piece, gate_ref[ins, where], preferred_element_type=F32)
                upward = upward + jnp.dot(piece, up_ref[ins, where], preferred_element_type=F32)
            hidden[:, where] = (jax.nn.silu(gate) * upward).astype(BF16)

        @pl.loop(0, tps)
        def _(t):
            where = pl.ds(pl.multiple_of(t * cols, cols), cols)
            done = jnp.dot(hidden[...], down_ref[:, where], preferred_element_type=F32)
            part[chunk, t % 2, t // 2] = done.astype(BF16)

    def pair_copy(chunk):
        return remote(
            part.at[chunk, 1 - core],
            pair_in.at[chunk],
            p_send.at[chunk],
            p_recv.at[chunk],
            {"tp": mate},
        )

    def cross_copy(chunk, j):
        return remote(
            pair_out.at[chunk, j - 1],
            ring_in.at[chunk, j - 1],
            q_send.at[chunk, j - 1],
            q_recv.at[chunk, j - 1],
            {"tp": ((tall + j) % halves) * 2 + core},
        )

    def cross(chunk):
        pair_copy(chunk).wait_recv()
        for j in range(1, halves):
            to = (tall + j) % halves
            total = part[chunk, core, to].astype(F32) + pair_in[chunk, to].astype(F32)
            pair_out[chunk, j - 1] = total.astype(BF16)
            go(cross_copy(chunk, j))

    def send_back(chunk):
        total = part[chunk, core, tall].astype(F32) + pair_in[chunk, tall].astype(F32)
        for j in range(1, halves):
            cross_copy(chunk, j).wait_recv()
            total = total + ring_in[chunk, j - 1].astype(F32)
        total = total.astype(BF16)
        each = count // chunks
        if chunk == 0:
            returned[0:cap, :] = total[0:cap]
        answer[chunk * size : (chunk + 1) * size, :] = total
        for k in range(chunk * each, (chunk + 1) * each):
            if k > 0:
                go(back_copy(k))

    def back_copy(k):
        return remote(
            answer.at[pl.ds(k * cap, cap), :],
            returned.at[pl.ds(k * cap, cap), :],
            r_send.at[k],
            r_recv.at[k],
            {"sp": (me + count - k) % count, "tp": mine},
        )

    for chunk in range(chunks):
        compute(chunk)
        go(pair_copy(chunk))
        if chunk > 0:
            send_back(chunk - 1)
        cross(chunk)
    send_back(chunks - 1)
    for k in range(1, count):
        back_copy(k).wait_recv()
    back = returned[...]
    total = jnp.dot(high_ref[...], back, preferred_element_type=F32)
    total = total + jnp.dot(low_ref[...], back, preferred_element_type=F32)
    out_ref[...] = (stream.astype(F32) + total).astype(BF16)
    for copy in pending:
        copy.wait_send()


def experts(stream, selector, high, low, gain, gate, up, down, cap):
    count = lax.axis_size("sp")
    tps = lax.axis_size("tp")
    halves = tps // 2
    tokens, cols = stream.shape
    slots = count * cap
    size = slots // 2
    batches = min(count, 8)
    vm = pl.BlockSpec(memory_space=pltpu.VMEM)
    hbm = pl.BlockSpec(memory_space=pl.ANY)
    dma = pltpu.SemaphoreType.DMA
    return pl.pallas_call(
        functools.partial(expert_kernel, count, tps, cap),
        out_shape=jax.ShapeDtypeStruct((tokens, cols), BF16),
        in_specs=[vm] * 5 + [hbm] * 3,
        out_specs=vm,
        scratch_shapes=[
            pltpu.VMEM(gate.shape[1:], BF16),
            pltpu.VMEM(up.shape[1:], BF16),
            pltpu.VMEM(down.shape[1:], BF16),
            pltpu.VMEM((slots, cols), BF16),
            pltpu.VMEM((tps, slots, cols), BF16),
            pltpu.VMEM((size, gate.shape[2]), BF16),
            pltpu.VMEM((2, 2, halves, size, cols), BF16),
            pltpu.VMEM((2, halves, size, cols), BF16),
            pltpu.VMEM((2, halves - 1, size, cols), BF16),
            pltpu.VMEM((2, halves - 1, size, cols), BF16),
            pltpu.VMEM((slots, cols), BF16),
            pltpu.VMEM((slots, cols), BF16),
            dma((3,)),
            dma((count,)),
            dma((count,)),
            dma((tps, batches)),
            dma((tps, batches)),
            dma((2,)),
            dma((2,)),
            dma((2, halves - 1)),
            dma((2, halves - 1)),
            dma((count,)),
            dma((count,)),
        ],
        compiler_params=pltpu.CompilerParams(
            collective_id=1, has_side_effects=True, vmem_limit_bytes=50 * 2**20
        ),
        name="experts",
    )(stream, selector, high, low, gain, gate, up, down)


def routes(couple, likelihood, scores, expert_total, capacity):
    tokens, top = couple.shape
    place = lax.axis_index("sp")
    turned = (couple + expert_total - place) % expert_total
    iota = lax.broadcasted_iota(jnp.int32, (tokens, top, expert_total), 2)
    hit = turned[:, :, None] == iota
    named = jnp.sum(hit.astype(jnp.float32), axis=1)
    lower = jnp.tril(jnp.ones((tokens, tokens), jnp.float32), -1)
    before = jnp.dot(lower, named, preferred_element_type=jnp.float32).astype(jnp.int32)
    rank = jnp.sum(jnp.where(hit, before[:, None, :], 0), axis=2)
    slot = turned * capacity + rank
    first = jax.nn.sigmoid(scores[:, 0] - scores[:, 1])
    weight = likelihood[:, None] * jnp.stack([first, 1.0 - first], axis=1)
    slots = expert_total * capacity
    lanes = lax.broadcasted_iota(jnp.int32, (tokens, slots), 1)
    mix = jnp.zeros((tokens, slots), jnp.float32)
    for k in range(top):
        mix = mix + jnp.where(slot[:, k : k + 1] == lanes, weight[:, k : k + 1], 0.0)
    high = mix.astype(jnp.bfloat16)
    low = (mix - high.astype(jnp.float32)).astype(jnp.bfloat16)
    column = lax.broadcasted_iota(jnp.int32, (slots, tokens), 0)
    flat = jnp.transpose(slot)
    chosen = (flat[0:1] == column) | (flat[1:2] == column)
    return chosen.astype(jnp.bfloat16), high, low


def body(
    skip_stream_entering,
    unfiltered_channel_feed,
    unfiltered_state_entry,
    unfiltered_state_exit,
    final_valve_preactivation,
    increment_preactivation,
    summed_attenuation_both_ways,
    channel_fading_speed,
    channel_feed_filter,
    state_entry_filter,
    state_exit_filter,
    clustered_rescale_factor,
    final_projection_weights,
    specialist_rescale_factor,
    item_specialist_couple,
    selected_cluster_likelihood,
    selected_twin_scores_raw,
    specialist_gating_weights,
    specialist_raising_weights,
    specialist_lowering_weights,
):
    tokens_here = skip_stream_entering.shape[0]
    heads_here = increment_preactivation.shape[1]
    x_width = unfiltered_channel_feed.shape[1]
    b_width = unfiltered_state_entry.shape[1]
    groups_here = b_width // NS
    joined = jnp.concatenate(
        [unfiltered_channel_feed, unfiltered_state_entry, unfiltered_state_exit], axis=1
    )
    padded = extended(joined, (("sp", 0),), CONV // 2)
    kernel = jnp.concatenate([channel_feed_filter, state_entry_filter, state_exit_filter], axis=1)
    summed = jnp.zeros(joined.shape, jnp.float32)
    for offset in range(CONV):
        summed = summed + kernel[offset] * padded[offset : offset + tokens_here].astype(jnp.float32)
    conv_out = jax.nn.silu(summed).astype(jnp.bfloat16)
    x_conv = conv_out[:, :x_width].reshape(tokens_here, heads_here, HD)
    b_conv = conv_out[:, x_width : x_width + b_width].reshape(tokens_here, groups_here, NS)
    c_conv = conv_out[:, x_width + b_width :].reshape(tokens_here, groups_here, NS)
    whole_increment_list = jax.nn.softplus(increment_preactivation)
    whole_attenuation_list = (
        -whole_increment_list * channel_fading_speed[:, :, None] + summed_attenuation_both_ways
    )
    within, state_fwd, state_bwd, total_fwd, total_bwd, factor_fwd, factor_bwd, c_head = (
        block_parts(
            x_conv,
            b_conv,
            c_conv,
            whole_increment_list[0],
            whole_increment_list[1],
            whole_attenuation_list[0],
            whole_attenuation_list[1],
        )
    )
    empty = (jnp.zeros_like(total_fwd), jnp.zeros_like(state_fwd))
    incoming_fwd = entering((total_fwd, state_fwd), "sp", compose, empty, False)[1]
    incoming_bwd = entering((total_bwd, state_bwd), "sp", compose, empty, True)[1]
    mixer_out = (
        within
        + read_state(c_head, factor_fwd, incoming_fwd)
        + read_state(c_head, factor_bwd, incoming_bwd)
    )
    gated = mixer_out.reshape(tokens_here, x_width) * jax.nn.silu(
        final_valve_preactivation.astype(jnp.float32)
    )
    grouped = gated.reshape(tokens_here, groups_here, -1)
    grouped = grouped * lax.rsqrt(jnp.mean(grouped * grouped, axis=-1, keepdims=True) + group_eps)
    mixed = (grouped.reshape(tokens_here, x_width) * clustered_rescale_factor).astype(jnp.bfloat16)
    projected = jnp.dot(
        lax.all_gather(mixed, "tp", axis=1, tiled=True),
        final_projection_weights,
        preferred_element_type=jnp.float32,
    )
    stream = (skip_stream_entering.astype(jnp.float32) + projected).astype(jnp.bfloat16)
    expert_total = lax.axis_size("sp")
    capacity = 4 * tokens_here // expert_total
    selector, high, low = routes(
        item_specialist_couple,
        selected_cluster_likelihood,
        selected_twin_scores_raw,
        expert_total,
        capacity,
    )
    return experts(
        stream,
        selector,
        high,
        low,
        specialist_rescale_factor[None, :],
        specialist_gating_weights,
        specialist_raising_weights,
        specialist_lowering_weights,
        capacity,
    )


def solution(mesh):
    placed = (
        P("sp", "tp"),
        P("sp", "tp"),
        P("sp", "tp"),
        P("sp", "tp"),
        P("sp", "tp"),
        P(None, "tp", "sp"),
        P(None, "tp", "sp"),
        P(None, "tp"),
        P(None, "tp"),
        P(None, "tp"),
        P(None, "tp"),
        P("tp"),
        P(None, "tp"),
        P(),
        P("sp", None),
        P("sp"),
        P("sp", None),
        P("sp", None, "tp"),
        P("sp", None, "tp"),
        P("sp", "tp", None),
    )
    return jax.shard_map(body, mesh=mesh, in_specs=placed, out_specs=P("sp", "tp"), check_vma=False)
```

```python
import functools

import jax
import jax.numpy as jnp
from jax import lax
from jax.experimental import pallas as pl
from jax.experimental.pallas import tpu as pltpu
from jax.sharding import PartitionSpec as P

HD = 64
NS = 128
CONV = 5


HIGHEST = lax.Precision.HIGHEST
group_eps = 1e-05
stream_eps = 1e-06


MESH = pl.DeviceIdType.MESH
F32 = jnp.float32
BF16 = jnp.bfloat16


def remote(src, dst, send, recv, device):
    return pltpu.make_async_remote_copy(
        src_ref=src, dst_ref=dst, send_sem=send, recv_sem=recv, device_id=device, device_id_type=MESH
    )


def expert_kernel(
    count,
    tps,
    cap,
    stream_ref,
    selector_ref,
    high_ref,
    low_ref,
    gain_ref,
    gate_hbm,
    up_hbm,
    down_hbm,
    out_ref,
    gate_ref,
    up_ref,
    down_ref,
    leaving,
    rows,
    hidden,
    part,
    pair_in,
    pair_out,
    ring_in,
    answer,
    returned,
    weight_sem,
    a_send,
    a_recv,
    b_send,
    b_recv,
    p_send,
    p_recv,
    q_send,
    q_recv,
    r_send,
    r_recv,
):
    me = lax.axis_index("sp")
    mine = lax.axis_index("tp")
    halves = tps // 2
    tall = mine // 2
    core = mine % 2
    mate = tall * 2 + (1 - core)
    cols = stream_ref.shape[1]
    loads = [
        pltpu.make_async_copy(gate_hbm.at[0], gate_ref, weight_sem.at[0]),
        pltpu.make_async_copy(up_hbm.at[0], up_ref, weight_sem.at[1]),
        pltpu.make_async_copy(down_hbm.at[0], down_ref, weight_sem.at[2]),
    ]
    for load in loads:
        load.start()

    barrier = pltpu.get_barrier_semaphore()
    for k in range(1, count):
        pl.semaphore_signal(
            barrier, inc=1, device_id={"sp": (me + k) % count, "tp": mine}, device_id_type=MESH
        )
    for j in range(1, tps):
        pl.semaphore_signal(
            barrier, inc=1, device_id={"sp": me, "tp": (mine + j) % tps}, device_id_type=MESH
        )
    stream = stream_ref[...]
    sent = jnp.dot(selector_ref[...], stream, preferred_element_type=F32).astype(BF16)
    leaving[...] = sent
    rows[mine, 0:cap, :] = sent[0:cap]
    pl.semaphore_wait(barrier, count + tps - 2)

    pending = []

    def go(copy):
        copy.start()
        pending.append(copy)

    for k in range(1, count):
        go(
            remote(
                leaving.at[pl.ds(k * cap, cap), :],
                rows.at[mine, pl.ds(k * cap, cap), :],
                a_send.at[k],
                a_recv.at[k],
                {"sp": (me + k) % count, "tp": mine},
            )
        )

    batches = min(count, 8)
    span = count // batches

    def area(owner, batch):
        return rows.at[owner, pl.ds(batch * span * cap, span * cap), :]

    def arrived_from(owner, batch, index):
        remote(
            area(owner, batch),
            area(owner, batch),
            b_send.at[index, batch],
            b_recv.at[index, batch],
            {"tp": mate},
        ).wait_recv()

    def relay(batch):
        for j in range(1, halves):
            owner = ((tall + halves - j) % halves) * 2 + core
            arrived_from(owner, batch, j)
            go(
                remote(
                    area(owner, batch),
                    area(owner, batch),
                    b_send.at[halves + j, batch],
                    b_recv.at[halves + j, batch],
                    {"tp": mate},
                )
            )

    for batch in range(batches):
        for k in range(batch * span, (batch + 1) * span):
            if k > 0:
                spot = rows.at[mine, pl.ds(k * cap, cap), :]
                remote(spot, spot, a_send.at[k], a_recv.at[k], {"tp": mate}).wait_recv()
        for j in range(1, halves):
            go(
                remote(
                    area(mine, batch),
                    area(mine, batch),
                    b_send.at[j, batch],
                    b_recv.at[j, batch],
                    {"tp": ((tall + j) % halves) * 2 + core},
                )
            )
        go(
            remote(
                area(mine, batch),
                area(mine, batch),
                b_send.at[halves, batch],
                b_recv.at[halves, batch],
                {"tp": mate},
            )
        )
        if batch > 0:
            relay(batch - 1)
    relay(batches - 1)
    for batch in range(batches):
        for j in range(halves):
            arrived_from(((tall + halves - j) % halves) * 2 + 1 - core, batch, halves + j)
    for copy in pending:
        copy.wait_send()
    pending = []

    chunks = 2
    size = count * cap // chunks
    units = gate_ref.shape[1]
    tile = min(256, units)
    for load in loads:
        load.wait()

    def compute(chunk):
        lo = chunk * size
        squares = jnp.zeros((size, 1), F32)
        for t in range(tps):
            piece = rows[t, lo : lo + size, :].astype(F32)
            squares = squares + jnp.sum(piece * piece, axis=1, keepdims=True)
        scale = lax.rsqrt(squares / (tps * cols) + stream_eps)
        for t in range(tps):
            piece = rows[t, lo : lo + size, :].astype(F32)
            gain = gain_ref[:, t * cols : (t + 1) * cols]
            rows[t, lo : lo + size, :] = (piece * scale * gain).astype(BF16)

        @pl.loop(0, units // tile)
        def _(step):
            where = pl.ds(pl.multiple_of(step * tile, tile), tile)
            gate = jnp.zeros((size, tile), F32)
            upward = jnp.zeros((size, tile), F32)
            for t in range(tps):
                piece = rows[t, lo : lo + size, :]
                ins = slice(t * cols, (t + 1) * cols)
                gate = gate + jnp.dot(piece, gate_ref[ins, where], preferred_element_type=F32)
                upward = upward + jnp.dot(piece, up_ref[ins, where], preferred_element_type=F32)
            hidden[:, where] = (jax.nn.silu(gate) * upward).astype(BF16)

        @pl.loop(0, tps)
        def _(t):
            where = pl.ds(pl.multiple_of(t * cols, cols), cols)
            done = jnp.dot(hidden[...], down_ref[:, where], preferred_element_type=F32)
            part[chunk, t % 2, t // 2] = done.astype(BF16)

    def pair_copy(chunk):
        return remote(
            part.at[chunk, 1 - core],
            pair_in.at[chunk],
            p_send.at[chunk],
            p_recv.at[chunk],
            {"tp": mate},
        )

    def cross_copy(chunk, j):
        return remote(
            pair_out.at[chunk, j - 1],
            ring_in.at[chunk, j - 1],
            q_send.at[chunk, j - 1],
            q_recv.at[chunk, j - 1],
            {"tp": ((tall + j) % halves) * 2 + core},
        )

    def cross(chunk):
        pair_copy(chunk).wait_recv()
        for j in range(1, halves):
            to = (tall + j) % halves
            total = part[chunk, core, to].astype(F32) + pair_in[chunk, to].astype(F32)
            pair_out[chunk, j - 1] = total.astype(BF16)
            go(cross_copy(chunk, j))

    def send_back(chunk):
        total = part[chunk, core, tall].astype(F32) + pair_in[chunk, tall].astype(F32)
        for j in range(1, halves):
            cross_copy(chunk, j).wait_recv()
            total = total + ring_in[chunk, j - 1].astype(F32)
        total = total.astype(BF16)
        each = count // chunks
        if chunk == 0:
            returned[0:cap, :] = total[0:cap]
        answer[chunk * size : (chunk + 1) * size, :] = total
        for k in range(chunk * each, (chunk + 1) * each):
            if k > 0:
                go(back_copy(k))

    def back_copy(k):
        return remote(
            answer.at[pl.ds(k * cap, cap), :],
            returned.at[pl.ds(k * cap, cap), :],
            r_send.at[k],
            r_recv.at[k],
            {"sp": (me + count - k) % count, "tp": mine},
        )

    for chunk in range(chunks):
        compute(chunk)
        go(pair_copy(chunk))
        if chunk > 0:
            send_back(chunk - 1)
        cross(chunk)
    send_back(chunks - 1)
    for k in range(1, count):
        back_copy(k).wait_recv()
    back = returned[...]
    total = jnp.dot(high_ref[...], back, preferred_element_type=F32)
    total = total + jnp.dot(low_ref[...], back, preferred_element_type=F32)
    out_ref[...] = (stream.astype(F32) + total).astype(BF16)
    for copy in pending:
        copy.wait_send()


def experts(stream, selector, high, low, gain, gate, up, down, cap):
    count = lax.axis_size("sp")
    tps = lax.axis_size("tp")
    halves = tps // 2
    tokens, cols = stream.shape
    slots = count * cap
    size = slots // 2
    batches = min(count, 8)
    vm = pl.BlockSpec(memory_space=pltpu.VMEM)
    hbm = pl.BlockSpec(memory_space=pl.ANY)
    dma = pltpu.SemaphoreType.DMA
    return pl.pallas_call(
        functools.partial(expert_kernel, count, tps, cap),
        out_shape=jax.ShapeDtypeStruct((tokens, cols), BF16),
        in_specs=[vm] * 5 + [hbm] * 3,
        out_specs=vm,
        scratch_shapes=[
            pltpu.VMEM(gate.shape[1:], BF16),
            pltpu.VMEM(up.shape[1:], BF16),
            pltpu.VMEM(down.shape[1:], BF16),
            pltpu.VMEM((slots, cols), BF16),
            pltpu.VMEM((tps, slots, cols), BF16),
            pltpu.VMEM((size, gate.shape[2]), BF16),
            pltpu.VMEM((2, 2, halves, size, cols), BF16),
            pltpu.VMEM((2, halves, size, cols), BF16),
            pltpu.VMEM((2, halves - 1, size, cols), BF16),
            pltpu.VMEM((2, halves - 1, size, cols), BF16),
            pltpu.VMEM((slots, cols), BF16),
            pltpu.VMEM((slots, cols), BF16),
            dma((3,)),
            dma((count,)),
            dma((count,)),
            dma((tps, batches)),
            dma((tps, batches)),
            dma((2,)),
            dma((2,)),
            dma((2, halves - 1)),
            dma((2, halves - 1)),
            dma((count,)),
            dma((count,)),
        ],
        compiler_params=pltpu.CompilerParams(
            collective_id=1, has_side_effects=True, vmem_limit_bytes=50 * 2**20
        ),
        name="experts",
    )(stream, selector, high, low, gain, gate, up, down)


def mixer_kernel(
    count,
    tps,
    feed_ref,
    entry_ref,
    exit_ref,
    valve_ref,
    increment_ref,
    attenuation_ref,
    speed_ref,
    feed_filter_ref,
    entry_filter_ref,
    exit_filter_ref,
    rescale_ref,
    skip_ref,
    weights_hbm,
    out_ref,
    weights_ref,
    halo,
    wide,
    table,
    states,
    totals,
    states_in,
    totals_in,
    carried,
    logs,
    mixed,
    weight_sem,
    h_send,
    h_recv,
    s_send,
    s_recv,
    t_send,
    t_recv,
    m_send,
    m_recv,
):
    me = lax.axis_index("sp")
    mine = lax.axis_index("tp")
    tokens, cols = feed_ref.shape
    heads = increment_ref.shape[1]
    group_count = cols // NS
    per = heads // group_count
    load = pltpu.make_async_copy(weights_hbm, weights_ref, weight_sem)
    load.start()
    barrier = pltpu.get_barrier_semaphore()
    for k in range(1, count):
        pl.semaphore_signal(
            barrier, inc=1, device_id={"sp": (me + k) % count, "tp": mine}, device_id_type=MESH
        )
    for j in range(1, tps):
        pl.semaphore_signal(
            barrier, inc=1, device_id={"sp": me, "tp": (mine + j) % tps}, device_id_type=MESH
        )

    sources = (feed_ref, entry_ref, exit_ref)
    filters = (feed_filter_ref, entry_filter_ref, exit_filter_ref)
    rim = halo.shape[2]

    def halo_copy(i, side):
        start = tokens - rim if side == 0 else 0
        to = (me + 1) % count if side == 0 else (me + count - 1) % count
        return remote(
            sources[i].at[pl.ds(start, rim), :],
            halo.at[side, i],
            h_send.at[side, i],
            h_recv.at[side, i],
            {"sp": to, "tp": mine},
        )

    up_to = me < count - 1
    down_to = me > 0
    pl.semaphore_wait(barrier, count + tps - 2)

    @pl.when(up_to)
    def _():
        for i in range(3):
            halo_copy(i, 0).start()

    @pl.when(down_to)
    def _():
        for i in range(3):
            halo_copy(i, 1).start()

    row = lax.broadcasted_iota(jnp.int32, (tokens, tokens), 0)
    col = lax.broadcasted_iota(jnp.int32, (tokens, tokens), 1)
    lower = col <= row
    diagonal = col == row
    raw = increment_ref[...]
    step = jnp.maximum(raw, 0.0) + jnp.log1p(jnp.exp(-jnp.abs(raw)))
    log = -step * speed_ref[...] + attenuation_ref[...]
    upto = jnp.where(row <= col, 1.0, 0.0).astype(F32)
    onward = jnp.where(row >= col, 1.0, 0.0).astype(F32)
    forward = jnp.dot(log[0], upto, precision=HIGHEST, preferred_element_type=F32)
    backward = jnp.dot(log[1], onward, precision=HIGHEST, preferred_element_type=F32)
    total_f = forward[:, tokens - 1 : tokens]
    total_b = backward[:, 0:1]
    table[...] = jnp.zeros(table.shape, F32)
    items = (
        forward,
        backward,
        jnp.exp(total_f - forward) * step[0],
        jnp.exp(total_b - backward) * step[1],
        jnp.exp(forward),
        jnp.exp(backward),
    )
    pitch = table.shape[0] // 8
    for q, item in enumerate(items):
        table[q * pitch : q * pitch + heads, :] = item
    turned = jnp.transpose(table[...])
    totals[...] = jnp.zeros(totals.shape, F32)
    totals[0, 0:heads, :] = jnp.broadcast_to(total_f, (heads, totals.shape[2]))
    totals[1, 0:heads, :] = jnp.broadcast_to(total_b, (heads, totals.shape[2]))
    lane_head = lax.broadcasted_iota(jnp.int32, (1, NS), 1) // HD

    def spread(q, g):
        first = g * per
        value = turned[:, q * pitch + first : q * pitch + first + 1]
        for i in range(1, per):
            at = q * pitch + first + i
            value = jnp.where(lane_head >= i, turned[:, at : at + 1], value)
        return value

    halo_zero = jnp.zeros((rim, cols), F32)

    @pl.when(down_to)
    def _():
        for i in range(3):
            halo_copy(i, 0).wait_recv()
            wide[i, 0:rim, :] = halo[0, i].astype(F32)

    @pl.when(me == 0)
    def _():
        for i in range(3):
            wide[i, 0:rim, :] = halo_zero

    @pl.when(up_to)
    def _():
        for i in range(3):
            halo_copy(i, 1).wait_recv()
            wide[i, rim + tokens : 2 * rim + tokens, :] = halo[1, i].astype(F32)

    @pl.when(me == count - 1)
    def _():
        for i in range(3):
            wide[i, rim + tokens : 2 * rim + tokens, :] = halo_zero

    short = []
    for i in range(3):
        wide[i, rim : rim + tokens, :] = sources[i][...].astype(F32)
        taps = filters[i][...]
        summed = jnp.zeros((tokens, cols), F32)
        for offset in range(CONV):
            begin = rim - CONV // 2 + offset
            summed = summed + taps[offset : offset + 1] * wide[i, begin : begin + tokens, :]
        short.append(jax.nn.silu(summed).astype(BF16))
    x_all, b_all, c_all = short
    across = (((0,), (0,)), ((), ()))
    along = (((1,), (1,)), ((), ()))
    for g in range(group_count):
        part = slice(g * NS, (g + 1) * NS)
        x_group = x_all[:, part].astype(F32)
        for way in range(2):
            weighted = (x_group * spread(2 + way, g)).astype(BF16)
            states[way, g] = lax.dot_general(
                weighted, b_all[:, part], across, preferred_element_type=F32
            ).astype(BF16)

    def state_copy(way, k):
        to = (me + k) % count if way == 0 else (me + count - k) % count
        return remote(
            states.at[way],
            states_in.at[way, k - 1],
            s_send.at[way, k - 1],
            s_recv.at[way, k - 1],
            {"sp": to, "tp": mine},
        )

    def total_copy(way, k):
        to = (me + k) % count if way == 0 else (me + count - k) % count
        return remote(
            totals.at[way],
            totals_in.at[way, k - 1],
            t_send.at[way, k - 1],
            t_recv.at[way, k - 1],
            {"sp": to, "tp": mine},
        )

    def sends(way, k):
        return me + k < count if way == 0 else me >= k

    def takes(way, k):
        return sends(1 - way, k)

    for k in range(1, count):
        for way in range(2):

            @pl.when(sends(way, k))
            def _(way=way, k=k):
                total_copy(way, k).start()
                state_copy(way, k).start()

    within = []
    for g in range(group_count):
        part = slice(g * NS, (g + 1) * NS)
        scores = lax.dot_general(
            c_all[:, part], b_all[:, part], along, preferred_element_type=F32
        )
        whole = None
        for i in range(per):
            h = g * per + i
            gap_f = turned[:, h : h + 1] - forward[h : h + 1, :]
            gap_b = turned[:, pitch + h : pitch + h + 1] - backward[h : h + 1, :]
            decay = jnp.exp(jnp.minimum(jnp.where(lower, gap_f, gap_b), 0.0))
            step_f = step[0, h : h + 1, :]
            step_b = step[1, h : h + 1, :]
            decay = decay * jnp.where(lower, step_f, step_b) + jnp.where(diagonal, step_b, 0.0)
            value = jnp.dot(
                (scores * decay).astype(BF16), x_all[:, part], preferred_element_type=F32
            )
            whole = value if whole is None else jnp.where(lane_head >= i, value, whole)
        within.append(whole)

    carried[...] = jnp.zeros(carried.shape, F32)
    logs[...] = jnp.zeros(logs.shape, F32)
    row_head = lax.broadcasted_iota(jnp.int32, (NS, 1), 0) // HD
    for k in range(1, count):
        for way in range(2):

            @pl.when(takes(way, k))
            def _(way=way, k=k):
                total_copy(way, k).wait_recv()
                state_copy(way, k).wait_recv()
                factor = jnp.exp(logs[way])
                for g in range(group_count):
                    scale = factor[g * per : g * per + 1, :]
                    for i in range(1, per):
                        at = g * per + i
                        scale = jnp.where(row_head >= i, factor[at : at + 1, :], scale)
                    carried[way, g] += states_in[way, k - 1, g].astype(F32) * scale
                logs[way] += totals_in[way, k - 1]

    for g in range(group_count):
        part = slice(g * NS, (g + 1) * NS)
        value = within[g]
        for way in range(2):
            read = lax.dot_general(
                c_all[:, part], carried[way, g].astype(BF16), along, preferred_element_type=F32
            )
            value = value + read * spread(4 + way, g)
        value = value * jax.nn.silu(valve_ref[:, part].astype(F32))
        value = value * lax.rsqrt(jnp.mean(value * value, axis=-1, keepdims=True) + group_eps)
        mixed[mine, :, part] = (value * rescale_ref[:, part]).astype(BF16)

    def mixed_copy(j):
        return remote(
            mixed.at[mine],
            mixed.at[mine],
            m_send.at[j - 1],
            m_recv.at[j - 1],
            {"sp": me, "tp": (mine + j) % tps},
        )

    for j in range(1, tps):
        mixed_copy(j).start()
    load.wait()

    def product(owner):
        ins = pl.ds(pl.multiple_of(owner * cols, cols), cols)
        return jnp.dot(mixed[owner], weights_ref[ins, :], preferred_element_type=F32)

    result = skip_ref[...].astype(F32) + product(mine)
    for j in range(1, tps):
        owner = (mine + tps - j) % tps
        spot = mixed.at[owner]
        remote(
            spot, spot, m_send.at[j - 1], m_recv.at[j - 1], {"sp": me, "tp": owner}
        ).wait_recv()
        result = result + product(owner)
    out_ref[...] = result.astype(BF16)

    for j in range(1, tps):
        mixed_copy(j).wait_send()
    for k in range(1, count):
        for way in range(2):

            @pl.when(sends(way, k))
            def _(way=way, k=k):
                total_copy(way, k).wait_send()
                state_copy(way, k).wait_send()

    @pl.when(up_to)
    def _():
        for i in range(3):
            halo_copy(i, 0).wait_send()

    @pl.when(down_to)
    def _():
        for i in range(3):
            halo_copy(i, 1).wait_send()


def mixer(feed, entry, leave, valve, inc, att, speed, taps, rescale, skip, weights):
    count = lax.axis_size("sp")
    tps = lax.axis_size("tp")
    tokens, cols = feed.shape
    group_count = cols // NS
    vm = pl.BlockSpec(memory_space=pltpu.VMEM)
    hbm = pl.BlockSpec(memory_space=pl.ANY)
    dma = pltpu.SemaphoreType.DMA
    rim = 16
    pitch = 16
    return pl.pallas_call(
        functools.partial(mixer_kernel, count, tps),
        out_shape=jax.ShapeDtypeStruct((tokens, cols), BF16),
        in_specs=[vm] * 12 + [hbm],
        out_specs=vm,
        scratch_shapes=[
            pltpu.VMEM(weights.shape, BF16),
            pltpu.VMEM((2, 3, rim, cols), BF16),
            pltpu.VMEM((3, tokens + 2 * rim, cols), F32),
            pltpu.VMEM((8 * pitch, tokens), F32),
            pltpu.VMEM((2, group_count, NS, NS), BF16),
            pltpu.VMEM((2, pitch, NS), F32),
            pltpu.VMEM((2, count - 1, group_count, NS, NS), BF16),
            pltpu.VMEM((2, count - 1, pitch, NS), F32),
            pltpu.VMEM((2, group_count, NS, NS), F32),
            pltpu.VMEM((2, pitch, NS), F32),
            pltpu.VMEM((tps, tokens, cols), BF16),
            dma,
            dma((2, 3)),
            dma((2, 3)),
            dma((2, count - 1)),
            dma((2, count - 1)),
            dma((2, count - 1)),
            dma((2, count - 1)),
            dma((tps - 1,)),
            dma((tps - 1,)),
        ],
        compiler_params=pltpu.CompilerParams(
            collective_id=2, has_side_effects=True, vmem_limit_bytes=40 * 2**20
        ),
        name="mixer",
    )(feed, entry, leave, valve, inc, att, speed, *taps, rescale, skip, weights)


def routes(couple, likelihood, scores, expert_total, capacity):
    tokens, top = couple.shape
    place = lax.axis_index("sp")
    turned = (couple + expert_total - place) % expert_total
    iota = lax.broadcasted_iota(jnp.int32, (tokens, top, expert_total), 2)
    hit = turned[:, :, None] == iota
    named = jnp.sum(hit.astype(jnp.float32), axis=1)
    lower = jnp.tril(jnp.ones((tokens, tokens), jnp.float32), -1)
    before = jnp.dot(lower, named, preferred_element_type=jnp.float32).astype(jnp.int32)
    rank = jnp.sum(jnp.where(hit, before[:, None, :], 0), axis=2)
    slot = turned * capacity + rank
    first = jax.nn.sigmoid(scores[:, 0] - scores[:, 1])
    weight = likelihood[:, None] * jnp.stack([first, 1.0 - first], axis=1)
    slots = expert_total * capacity
    lanes = lax.broadcasted_iota(jnp.int32, (tokens, slots), 1)
    mix = jnp.zeros((tokens, slots), jnp.float32)
    for k in range(top):
        mix = mix + jnp.where(slot[:, k : k + 1] == lanes, weight[:, k : k + 1], 0.0)
    high = mix.astype(jnp.bfloat16)
    low = (mix - high.astype(jnp.float32)).astype(jnp.bfloat16)
    column = lax.broadcasted_iota(jnp.int32, (slots, tokens), 0)
    flat = jnp.transpose(slot)
    chosen = (flat[0:1] == column) | (flat[1:2] == column)
    return chosen.astype(jnp.bfloat16), high, low


def body(
    skip_stream_entering,
    unfiltered_channel_feed,
    unfiltered_state_entry,
    unfiltered_state_exit,
    final_valve_preactivation,
    increment_preactivation,
    summed_attenuation_both_ways,
    channel_fading_speed,
    channel_feed_filter,
    state_entry_filter,
    state_exit_filter,
    clustered_rescale_factor,
    final_projection_weights,
    specialist_rescale_factor,
    item_specialist_couple,
    selected_cluster_likelihood,
    selected_twin_scores_raw,
    specialist_gating_weights,
    specialist_raising_weights,
    specialist_lowering_weights,
):
    tokens_here = skip_stream_entering.shape[0]
    stream = mixer(
        unfiltered_channel_feed,
        unfiltered_state_entry,
        unfiltered_state_exit,
        final_valve_preactivation,
        increment_preactivation,
        summed_attenuation_both_ways,
        channel_fading_speed[:, :, None],
        (channel_feed_filter, state_entry_filter, state_exit_filter),
        clustered_rescale_factor[None, :],
        skip_stream_entering,
        final_projection_weights,
    )
    expert_total = lax.axis_size("sp")
    capacity = 4 * tokens_here // expert_total
    selector, high, low = routes(
        item_specialist_couple,
        selected_cluster_likelihood,
        selected_twin_scores_raw,
        expert_total,
        capacity,
    )
    return experts(
        stream,
        selector,
        high,
        low,
        specialist_rescale_factor[None, :],
        specialist_gating_weights,
        specialist_raising_weights,
        specialist_lowering_weights,
        capacity,
    )


def solution(mesh):
    placed = (
        P("sp", "tp"),
        P("sp", "tp"),
        P("sp", "tp"),
        P("sp", "tp"),
        P("sp", "tp"),
        P(None, "tp", "sp"),
        P(None, "tp", "sp"),
        P(None, "tp"),
        P(None, "tp"),
        P(None, "tp"),
        P(None, "tp"),
        P("tp"),
        P(None, "tp"),
        P(),
        P("sp", None),
        P("sp"),
        P("sp", None),
        P("sp", None, "tp"),
        P("sp", None, "tp"),
        P("sp", "tp", None),
    )
    return jax.shard_map(body, mesh=mesh, in_specs=placed, out_specs=P("sp", "tp"), check_vma=False)
```
